256 devices in a mesh: grp: 2 (over y), fs: 16 (over z), tp: 8 (over x, core).
Axes of the slice: x: 4, y: 2, z: 16, core: 2. Of those that a mesh axis runs over, the one named last changes fastest.
The devices are a block of a 4x16x16 slice.
Arguments:
- tokens: bfloat16 [24576, 2048], P(('grp', 'fs'), 'tp'), parts along dimension 0, may hold values from -6 to 6
- recurrent_norm_gain: float32 [2048], replicated, may hold values from 0.1 to 1.9
- channel_norm_gain: float32 [2048], replicated, may hold values from 0.1 to 1.9
- gate_projection_weight: float32 [2048, 2048], P('fs', 'tp'), may hold values from -0.125 to 0.125
- gate_column_scale: float32 [2048], P(('tp', 'fs')), may hold values from 0.5 to 2
- input_projection_weight: float32 [2048, 2048], P('fs', 'tp'), may hold values from -0.125 to 0.125
- input_column_scale: float32 [2048], P(('tp', 'fs')), may hold values from 0.5 to 2
- convolution_kernel: float32 [4, 2048], P(None, 'tp'), may hold values from -3 to 3
- recurrence_gate_weight: float32 [8, 256, 256], P('tp', 'fs'), may hold values from -0.375 to 0.375
- recurrence_column_scale: float32 [8, 256], P('tp', 'fs'), may hold values from 0.25 to 4
- input_gate_weight: float32 [8, 256, 256], P('tp', 'fs'), may hold values from -0.375 to 0.375
- input_gate_column_scale: float32 [8, 256], P('tp', 'fs'), may hold values from 0.5 to 2
- channel_decay_param: float32 [2048], P('tp'), may hold values from 2.2 to 8.5
- position_decay_shift: float32 [24576], P(('grp', 'fs')), parts along dimension 0, may hold values from -0.7 to 0
- output_projection_weight: float32 [2048, 2048], P('tp', 'fs'), may hold values from -0.125 to 0.125
- output_column_scale: float32 [2048], P('fs'), may hold values from 0.5 to 2
- mixer_gate_weight: float32 [2048, 5632], P('fs', 'tp'), may hold values from -0.125 to 0.125
- mixer_gate_column_scale: float32 [5632], P(('tp', 'fs')), may hold values from 0.5 to 2
- up_projection_weight: float32 [2048, 5632], P('fs', 'tp'), may hold values from -0.125 to 0.125
- up_column_scale: float32 [5632], P(('tp', 'fs')), may hold values from 0.5 to 2
- down_projection_weight: float32 [5632, 2048], P('tp', 'fs'), may hold values from -0.078125 to 0.078125
- down_column_scale: float32 [2048], P('fs'), may hold values from 0.5 to 2
Outputs:
- layer_out: bfloat16 [24576, 2048], P(('grp', 'fs'), 'tp'), parts along dimension 0
The draws below stay inside these ranges and needn't reach their ends.
There are 2 independent parts, one for each index of `grp`. The reference program is written for one: setup_inputs(seed, part) draws one part's arguments, and reference() takes and returns one part's arrays. A program takes and returns all parts, laid end to end along the dimension named above; an argument that names none is the same for every part. Nothing has to cross between parts.
All inputs are finite; a program needn't handle non-finite values.
Results may differ from the reference program's by a relative error of at most 0.023.
Values may be sent and summed in bfloat16 or wider, within the bound.
No kernel may reach another device: no remote copies, remote signals or barrier semaphores. Data moves between devices by JAX's collectives and lax.ppermute only.
A program may use at most 64 MiB of HBM per device.

```python
import math
import jax
import jax.numpy as jnp
from jax import lax

D = 2048
LRU = 2048
BW = 256
FF = 5632
TAPS = 4
SEQ_LEN = 128
BLOCKS = 8
TOKENS = 12288
N_TP = 8


def draw_channel_decay_param(key, part):
    pick_key, slow_key, fast_key = jax.random.split(jax.random.fold_in(key, 11), 3)
    fast_share = 0.5
    is_fast = jax.random.uniform(pick_key, (LRU,), jnp.float32) < fast_share
    slow_rate = jnp.exp(jax.random.uniform(slow_key, (LRU,), jnp.float32, jnp.log(0.05 / SEQ_LEN), jnp.log(0.3 / SEQ_LEN)))
    fast_rate = jnp.exp(jax.random.uniform(fast_key, (LRU,), jnp.float32, jnp.log(0.03), jnp.log(0.1)))
    rate = jnp.where(is_fast, fast_rate, slow_rate)
    return -jnp.log(jnp.expm1(rate))


def draw_position_decay_shift(key, part):
    place_key, depth_key = jax.random.split(jax.random.fold_in(key, 23))
    seq_count = TOKENS // SEQ_LEN
    places = jax.random.randint(place_key, (seq_count, 1, 4), 1, SEQ_LEN)
    within = jnp.arange(SEQ_LEN)[None, :, None]
    struck = jnp.any(within == places, axis=2)
    depth = jax.random.uniform(depth_key, (seq_count, SEQ_LEN), jnp.float32, jnp.log(0.5), jnp.log(0.8))
    return jnp.where(struck, depth, 0.0).reshape(TOKENS)


def level_of(stream_key, dims, pieces, low, top_value):
    gain, own = 1.0, jax.random.fold_in(stream_key, 6)
    for dim, parts in pieces:
        draws = jnp.exp(jax.random.uniform(jax.random.fold_in(own, dim), (parts,), jnp.float32, low / len(pieces), top_value / len(pieces)))
        gain = gain * jnp.repeat(draws, dims[dim] // parts).reshape([-1 if axis == dim else 1 for axis in range(len(dims))])
    return gain


def centred(stream_key, extent, width, bound, cuts=(), dtype=jnp.bfloat16):
    array = width * jax.random.normal(stream_key, extent, jnp.float32)
    if cuts:
        array = array * level_of(stream_key, extent, cuts, -0.22, 0.18)
    return jnp.clip(array, -bound, bound).astype(dtype)


def setup_inputs(seed: int = 0, part: int = 0) -> dict:
    arg_keys = jax.random.split(jax.random.key(seed), 23)
    own_keys = jax.random.split(jax.random.fold_in(arg_keys[22], part), 23)
    tokens = centred(own_keys[0], (TOKENS, D), 1.0, 6.0, ((0, 16), (1, 8)))
    recurrent_norm_gain = jnp.clip(1.0 + 0.18 * jax.random.normal(arg_keys[1], (D,), jnp.float32), 0.1, 1.9)
    channel_norm_gain = jnp.clip(1.0 + 0.18 * jax.random.normal(arg_keys[2], (D,), jnp.float32), 0.1, 1.9)
    gate_projection_weight = centred(arg_keys[3], (D, LRU), D ** -0.5, 0.125, ((0, 16), (1, 8)), jnp.float32)
    gate_column_scale = jnp.clip(jnp.exp(math.log(2.0) - 1.3862944 * jax.random.uniform(arg_keys[4], (LRU,), jnp.float32) ** level_of(arg_keys[4], (LRU,), ((0, 128),), -0.2, 0.2)), 0.5, 2.0)
    input_projection_weight = centred(arg_keys[5], (D, LRU), D ** -0.5, 0.125, ((0, 16), (1, 8)), jnp.float32)
    input_column_scale = jnp.clip(jnp.exp(math.log(2.0) - 1.3862944 * jax.random.uniform(arg_keys[6], (LRU,), jnp.float32) ** level_of(arg_keys[6], (LRU,), ((0, 128),), -0.2, 0.2)), 0.5, 2.0)
    convolution_kernel = centred(arg_keys[7], (TAPS, LRU), 0.5, 3.0, ((1, 8),), jnp.float32)
    recurrence_gate_weight = centred(arg_keys[8], (BLOCKS, BW, BW), BW ** -0.5, 0.375, ((0, 8), (1, 16)), jnp.float32)
    recurrence_column_scale = jnp.clip(jnp.exp(math.log(4.0) - 2.7725887 * jax.random.uniform(arg_keys[9], (BLOCKS, BW), jnp.float32) ** level_of(arg_keys[9], (BLOCKS, BW), ((0, 8), (1, 16)), -0.2, 0.2)), 0.25, 4.0)
    input_gate_weight = centred(arg_keys[10], (BLOCKS, BW, BW), BW ** -0.5, 0.375, ((0, 8), (1, 16)), jnp.float32)
    input_gate_column_scale = jnp.clip(jnp.exp(math.log(2.0) - 1.3862944 * jax.random.uniform(arg_keys[11], (BLOCKS, BW), jnp.float32) ** level_of(arg_keys[11], (BLOCKS, BW), ((0, 8), (1, 16)), -0.2, 0.2)), 0.5, 2.0)
    channel_decay_param = draw_channel_decay_param(jax.random.fold_in(arg_keys[22], 71), part)
    position_decay_shift = draw_position_decay_shift(jax.random.fold_in(jax.random.fold_in(arg_keys[22], part), 71), part)
    output_projection_weight = centred(arg_keys[14], (LRU, D), LRU ** -0.5, 0.125, ((0, 8), (1, 16)), jnp.float32)
    output_column_scale = jnp.clip(jnp.exp(math.log(2.0) - 1.3862944 * jax.random.uniform(arg_keys[15], (D,), jnp.float32) ** level_of(arg_keys[15], (D,), ((0, 16),), -0.2, 0.2)), 0.5, 2.0)
    mixer_gate_weight = centred(arg_keys[16], (D, FF), D ** -0.5, 0.125, ((0, 16), (1, 8)), jnp.float32)
    mixer_gate_column_scale = jnp.clip(jnp.exp(math.log(2.0) - 1.3862944 * jax.random.uniform(arg_keys[17], (FF,), jnp.float32) ** level_of(arg_keys[17], (FF,), ((0, 128),), -0.2, 0.2)), 0.5, 2.0)
    up_projection_weight = centred(arg_keys[18], (D, FF), D ** -0.5, 0.125, ((0, 16), (1, 8)), jnp.float32)
    up_column_scale = jnp.clip(jnp.exp(math.log(2.0) - 1.3862944 * jax.random.uniform(arg_keys[19], (FF,), jnp.float32) ** level_of(arg_keys[19], (FF,), ((0, 128),), -0.2, 0.2)), 0.5, 2.0)
    down_projection_weight = centred(arg_keys[20], (FF, D), FF ** -0.5, 0.078125, ((0, 8), (1, 16)), jnp.float32)
    down_column_scale = jnp.clip(jnp.exp(math.log(2.0) - 1.3862944 * jax.random.uniform(arg_keys[21], (D,), jnp.float32) ** level_of(arg_keys[21], (D,), ((0, 16),), -0.2, 0.2)), 0.5, 2.0)
    return {"tokens": tokens, "recurrent_norm_gain": recurrent_norm_gain, "channel_norm_gain": channel_norm_gain, "gate_projection_weight": gate_projection_weight, "gate_column_scale": gate_column_scale, "input_projection_weight": input_projection_weight, "input_column_scale": input_column_scale, "convolution_kernel": convolution_kernel, "recurrence_gate_weight": recurrence_gate_weight, "recurrence_column_scale": recurrence_column_scale, "input_gate_weight": input_gate_weight, "input_gate_column_scale": input_gate_column_scale, "channel_decay_param": channel_decay_param, "position_decay_shift": position_decay_shift, "output_projection_weight": output_projection_weight, "output_column_scale": output_column_scale, "mixer_gate_weight": mixer_gate_weight, "mixer_gate_column_scale": mixer_gate_column_scale, "up_projection_weight": up_projection_weight, "up_column_scale": up_column_scale, "down_projection_weight": down_projection_weight, "down_column_scale": down_column_scale}


eps = 1e-06

def rms_rows(row_block, gain_vec):
    widened = row_block.astype(jnp.float32)
    scaled = widened * lax.rsqrt(lax.optimization_barrier(jnp.mean(widened * widened, axis=-1, keepdims=True)) + eps)
    return (scaled * gain_vec).astype(jnp.bfloat16)

def project(row_block, weight, column_scale):
    return jnp.dot(row_block, weight.astype(jnp.bfloat16), preferred_element_type=jnp.float32) * column_scale

def grouped_sum(row_block, weight, column_scale):
    group_width = row_block.shape[1] // N_TP
    summed = jnp.zeros((row_block.shape[0], weight.shape[1]), jnp.float32)
    for member in range(N_TP):
        first_col = member * group_width
        partial_term = project(row_block[:, first_col:first_col + group_width], weight[first_col:first_col + group_width], column_scale)
        summed = summed + lax.optimization_barrier(partial_term.astype(jnp.bfloat16)).astype(jnp.float32)
    return summed

def convolve(branch, convolution_kernel):
    row_count, channels = branch.shape
    framed = branch.astype(jnp.float32).reshape(row_count // SEQ_LEN, SEQ_LEN, channels)
    padded = jnp.pad(framed, ((0, 0), (TAPS - 1, 0), (0, 0)))
    summed = jnp.zeros_like(framed)
    for offset in range(TAPS):
        summed = summed + padded[:, TAPS - 1 - offset:TAPS - 1 - offset + SEQ_LEN] * convolution_kernel[offset]
    return summed.reshape(row_count, channels).astype(jnp.bfloat16)

def block_gate(convolved_output, weight, column_scale):
    row_count = convolved_output.shape[0]
    framed = convolved_output.astype(jnp.float32).reshape(row_count, weight.shape[0], weight.shape[1])
    rounded = lax.optimization_barrier(weight.astype(jnp.bfloat16)).astype(jnp.float32)
    preact = jnp.einsum('tni,nio->tno', framed, rounded) * column_scale
    return jax.nn.sigmoid(preact).reshape(row_count, -1)

def carried_state(convolved_output, recurrence_gate_value, input_gate_value, channel_decay_param, position_decay_shift):
    row_count, channels = convolved_output.shape
    log_retention = -8.0 * recurrence_gate_value * jax.nn.softplus(-channel_decay_param) + position_decay_shift[:, None]
    starts = (jnp.arange(row_count) % SEQ_LEN == 0)[:, None]
    factor = jnp.where(starts, 1.0, jnp.sqrt(-jnp.expm1(2.0 * log_retention)))
    drive = convolved_output.astype(jnp.float32) * input_gate_value * factor
    framed_shape = (row_count // SEQ_LEN, SEQ_LEN, channels)

    def combine(earlier, later):
        return (earlier[0] * later[0], later[0] * earlier[1] + later[1])
    _, hidden_states = lax.associative_scan(combine, (jnp.exp(log_retention).reshape(framed_shape), drive.reshape(framed_shape)), axis=1)
    return hidden_states.reshape(row_count, channels)

def reference(tokens, recurrent_norm_gain, channel_norm_gain, gate_projection_weight, gate_column_scale, input_projection_weight, input_column_scale, convolution_kernel, recurrence_gate_weight, recurrence_column_scale, input_gate_weight, input_gate_column_scale, channel_decay_param, position_decay_shift, output_projection_weight, output_column_scale, mixer_gate_weight, mixer_gate_column_scale, up_projection_weight, up_column_scale, down_projection_weight, down_column_scale):
    normed = rms_rows(tokens, recurrent_norm_gain)
    gate_branch = project(normed, gate_projection_weight, gate_column_scale).astype(jnp.bfloat16)
    input_branch = project(normed, input_projection_weight, input_column_scale).astype(jnp.bfloat16)
    convolved_output = convolve(input_branch, convolution_kernel)
    recurrence_gate_value = block_gate(convolved_output, recurrence_gate_weight, recurrence_column_scale)
    input_gate_value = block_gate(convolved_output, input_gate_weight, input_gate_column_scale)
    hidden_states = carried_state(convolved_output, recurrence_gate_value, input_gate_value, channel_decay_param, position_decay_shift)
    mixer_rows = (jax.nn.gelu(gate_branch.astype(jnp.float32)) * hidden_states).astype(jnp.bfloat16)
    mixer_sum = grouped_sum(mixer_rows, output_projection_weight, output_column_scale)
    hidden = (tokens.astype(jnp.float32) + mixer_sum).astype(jnp.bfloat16)
    channel_normed = rms_rows(hidden, channel_norm_gain)
    swish_pre = project(channel_normed, mixer_gate_weight, mixer_gate_column_scale)
    upward_pre = project(channel_normed, up_projection_weight, up_column_scale)
    activation = (jax.nn.silu(swish_pre) * upward_pre).astype(jnp.bfloat16)
    channel_sum = grouped_sum(activation, down_projection_weight, down_column_scale)
    return (hidden.astype(jnp.float32) + channel_sum).astype(jnp.bfloat16)
```

```python
import functools

import jax
import jax.numpy as jnp
import numpy as np
from jax import lax
from jax.experimental import pallas as pl
from jax.experimental.pallas import tpu as pltpu
from jax.sharding import PartitionSpec as P

SEQ_LEN = 128
EPS = 1e-06
F32 = jnp.float32
BF16 = jnp.bfloat16


def fs_ring(size):
    forward = [(i, (i + 1) % size) for i in range(size)]
    backward = [(i, (i - 1) % size) for i in range(size)]
    return forward, backward


def ring_step(up, down, step, size):
    forward, backward = fs_ring(size)
    up = lax.ppermute(up, "fs", forward)
    return up, (lax.ppermute(down, "fs", backward) if step < size - step else None)


def after(value, *events):
    return lax.optimization_barrier((value, *events))[0]


def tp_perms(size):
    chips = size // 2
    swap = [(i, i ^ 1) for i in range(size)]
    lane = [(i, ((i // 2 + (1 if i % 2 == 0 else -1)) % chips) * 2 + i % 2) for i in range(size)]
    return swap, lane


def tp_gather(own, size):
    swap, lane = tp_perms(size)
    near = lax.ppermute(own, "tp", lane)
    partner = lax.ppermute(own, "tp", swap)
    near_other = lax.ppermute(partner, "tp", lane)
    far = lax.ppermute(near, "tp", lane)
    return [
        own,
        partner,
        near,
        near_other,
        far,
        lax.ppermute(near, "tp", swap),
        lax.ppermute(near_other, "tp", swap),
        lax.ppermute(far, "tp", swap),
    ]


def gather_order(index, size):
    chips = size // 2
    chip, core = index // 2, index % 2
    sign = 1 - 2 * core
    behind, ahead = (chip - sign) % chips, (chip + sign) % chips
    across = (chip + 2) % chips
    return [
        2 * chip + core,
        2 * chip + 1 - core,
        2 * behind + core,
        2 * behind + 1 - core,
        2 * across + core,
        2 * ahead + 1 - core,
        2 * ahead + core,
        2 * across + 1 - core,
    ]


def scatter_order(index, size):
    chips = size // 2
    chip, core = index // 2, index % 2
    sign = 1 - 2 * core
    ahead, behind = (chip + sign) % chips, (chip - sign) % chips
    across = (chip + 2) % chips
    return [
        2 * across + 1 - core,
        2 * behind + 1 - core,
        2 * behind + core,
        2 * chip + 1 - core,
        2 * across + core,
        2 * ahead + core,
        2 * ahead + 1 - core,
        2 * chip + core,
    ]


def tables(groups, fs, tp):
    rows = []
    for g in range(groups):
        for z in range(fs):
            for t in range(tp):
                order = gather_order(t, tp)
                blocks = [(z - (2 * p + h)) % fs for p in order for h in range(2)]
                where = np.argsort(scatter_order(t, tp))
                absolute = [(z - j) % fs for j in range(fs)]
                laid = [2 * int(where[a // 2]) + a % 2 for a in absolute]
                rows.append(order + blocks + laid + [16 * a for a in absolute] + [64 * (g % 2), z])
    return np.asarray(rows, np.int32).reshape(groups, fs, tp, -1)


def tp_scatter(partial, size, events):
    swap, lane = tp_perms(size)
    given_far, given_rest, kept = partial
    taken_far = lax.ppermute(given_far, "tp", swap)
    taken = lax.ppermute(given_rest, "tp", swap)
    events["swapped"] = taken_far
    far = lax.ppermute((kept[0:2].astype(F32) + taken_far.astype(F32)).astype(BF16), "tp", lane)
    other = lax.ppermute((kept[4:6].astype(F32) + taken[2:4].astype(F32)).astype(BF16), "tp", lane)
    events["far"] = far
    near = kept[2:4].astype(F32) + taken[0:2].astype(F32)
    mine = lax.ppermute((near + far.astype(F32)).astype(BF16), "tp", lane)
    other = lax.ppermute(other, "tp", swap)
    return kept, taken, mine, other


def add_body(base, kept, taken, mine, other, out):
    for half in range(2):
        lanes = slice(128 * half, 128 * half + 128)
        total = kept[half].astype(F32) + taken[half].astype(F32)
        total = total + mine[half].astype(F32) + other[half].astype(F32)
        out[:, lanes] = (base[:, lanes].astype(F32) + total).astype(BF16)


def add_terms(base, terms):
    rows = base.shape[0]
    step = rows // 2

    def pair(k):
        return pl.BlockSpec((2, step, 128), lambda i: (k, i, 0))

    flat = pl.BlockSpec((step, 256), lambda i: (i, 0))
    return pl.pallas_call(
        add_body,
        grid=(rows // step,),
        in_specs=[flat, pair(3), pair(2), pair(0), pair(0)],
        out_specs=flat,
        out_shape=jax.ShapeDtypeStruct(base.shape, BF16),
        compiler_params=pltpu.CompilerParams(vmem_limit_bytes=8 << 20),
        cost_estimate=pl.CostEstimate(flops=rows * 256 * 2000, bytes_accessed=rows * 256 * 12, transcendentals=0),
    )(base, *terms)


def norm_into(order, gain, shards, xs, rows):
    width = shards[0].shape[1] * len(shards)
    square = None
    for shard in shards:
        v = shard[rows, :].astype(F32)
        s = v * v
        s = s[:, :128] + s[:, 128:]
        square = s if square is None else square + s
    inverse = lax.rsqrt(jnp.sum(square, axis=1, keepdims=True) * (1.0 / width) + EPS)
    for n, shard in enumerate(shards):
        v = shard[rows, :].astype(F32) * inverse * gain[order[n]]
        v = v.astype(BF16)
        for half in range(2):
            xs[order[8 + 2 * n + half]] = v[:, 128 * half : 128 * half + 128]


def lay_down(order, laid, rows, left, right, count):
    for j in range(0, count, 2):
        columns = slice(128 * j, 128 * j + 256)
        result = jnp.dot(left, right[:, columns], preferred_element_type=F32).astype(BF16)
        laid[order[24 + j], rows, :] = result[:, :128]
        laid[order[24 + j + 1], rows, :] = result[:, 128:]


STEP = 3 * SEQ_LEN


def recurrent_body(count, order, gain, taps, decay, shift, *refs):
    shards, refs = refs[:8], refs[8:]
    firsts, refs = refs[:count], refs[count:]
    given_far, given, kept, passed, xs, weight, gates, out, laid = refs
    total = laid.shape[1]
    depth = weight.shape[0] // count
    fourth = gates.shape[0] // 4
    scales = None
    for j, first in enumerate(firsts):
        weight[depth * j : depth * (j + 1), :] = first[:depth, :]
        at = pl.multiple_of(order[40 + j], 16)
        gates[pl.ds(at, 16), :] = first[depth : depth + 16, :]
        part = first[depth + 16 : depth + 32, :].astype(F32)
        scales = part if scales is None else scales + part
        for q in range(4):
            block = first[depth + 32 : depth + 32 + fourth, 128 * q : 128 * q + 128]
            out[fourth * q : fourth * (q + 1), 128 * j : 128 * j + 128] = block
    passed[...] = scales
    branch_scale = scales[0:1] + scales[1:2]
    gate_scale = scales[2:3] + scales[3:4]

    def chunk(r, carry):
        rows = pl.ds(pl.multiple_of(r * STEP, STEP), STEP)
        norm_into(order, gain, shards, xs, rows)
        left = jnp.concatenate([xs[j] for j in range(count)], axis=1)
        sums = jnp.dot(left, weight[...], preferred_element_type=F32) * branch_scale
        gate_branch = sums[:, :256].astype(BF16).astype(F32)
        branch = sums[:, 256:].astype(BF16).astype(F32)
        place = lax.broadcasted_iota(jnp.int32, (STEP, 256), 0) % SEQ_LEN
        conv = branch * taps[0:1, :]
        for k in range(1, 4):
            moved = jnp.where(place >= k, pltpu.roll(branch, k, 0), 0.0)
            conv = conv + moved * taps[k : k + 1, :]
        conv16 = conv.astype(BF16)
        conv = conv16.astype(F32)
        both = jnp.dot(conv16, gates[...], preferred_element_type=F32) * gate_scale
        both = 1.0 / (1.0 + jnp.exp(-both))
        log_keep = both[:, :256] * decay[...] + shift[rows, :]
        twice = 2.0 * log_keep
        series = 1.0 + twice * (1.0 / 7)
        for d in (6, 5, 4, 3, 2):
            series = 1.0 + twice * (1.0 / d) * series
        lost = jnp.where(twice > -0.35, -twice * series, 1.0 - jnp.exp(twice))
        first = place == 0
        state = conv * both[:, 256:] * jnp.where(first, 1.0, jnp.sqrt(lost))
        keep = jnp.where(first, 0.0, jnp.exp(log_keep))
        d = 1
        while d < SEQ_LEN:
            state = state + keep * pltpu.roll(state, d, 0)
            if 2 * d < SEQ_LEN:
                keep = keep * pltpu.roll(keep, d, 0)
            d *= 2
        mixed = (jax.nn.gelu(gate_branch) * state).astype(BF16)
        lay_down(order, laid, rows, mixed, out, count)
        return carry

    lax.fori_loop(0, total // STEP, chunk, 0)
    given_far[...] = laid[:2]
    given[...] = laid[2:8]
    kept[...] = laid[8:]


def mixer_body(count, batches, order, gain, scales, *refs):
    shards, refs = refs[:8], refs[8:]
    pieces, refs = refs[:count], refs[count:]
    swapped, refs = refs[: len(batches)], refs[len(batches) :]
    given_far, given, kept, xs, weight, down, laid = refs
    total = laid.shape[1]
    half = weight.shape[0] // count // 2
    wide = weight.shape[1]
    main = (wide - 128) // 2
    own = pl.multiple_of(order[56], half)
    lanes = wide // 128
    for j, piece in enumerate(pieces):
        weight[pl.ds(2 * half * j + own, half), :] = piece[:half, :]
        columns = slice(128 * j, 128 * j + 128)
        for q in range(lanes):
            at = half * (q if q < lanes - 1 else q + 1)
            down[at : at + half, columns] = piece[half:, 128 * q : 128 * q + 128]
        down[main : main + half, columns] = jnp.zeros((half, 128), BF16)
    for batch, group in zip(swapped, batches):
        for i, j in enumerate(group):
            weight[pl.ds(2 * half * j + half - own, half), :] = batch[half * i : half * (i + 1), :]
    at = [scales[4 + k : 5 + k, :] + scales[7 + k : 8 + k, :] for k in range(3)]
    scale = jnp.concatenate(at, axis=1)[:, :wide]

    def chunk(r, carry):
        rows = pl.ds(pl.multiple_of(r * STEP, STEP), STEP)
        norm_into(order, gain, shards, xs, rows)
        left = jnp.concatenate([xs[j] for j in range(count)], axis=1)
        sums = jnp.dot(left, weight[...], preferred_element_type=F32) * scale
        swish, upward, tail = sums[:, :main], sums[:, main : 2 * main], sums[:, 2 * main :]
        active = (swish / (1.0 + jnp.exp(-swish)) * upward).astype(BF16)
        turned = pltpu.roll(tail, 64, 1)
        lane = lax.broadcasted_iota(jnp.int32, tail.shape, 1)
        last = jnp.where(lane >= 64, turned / (1.0 + jnp.exp(-turned)) * tail, 0.0).astype(BF16)
        active = jnp.concatenate([active, last], axis=1)
        lay_down(order, laid, rows, active, down, count)
        return carry

    lax.fori_loop(0, total // STEP, chunk, 0)
    given_far[...] = laid[:2]
    given[...] = laid[2:8]
    kept[...] = laid[8:]


def vmem():
    return pl.BlockSpec(memory_space=pltpu.VMEM)


def smem():
    return pl.BlockSpec(memory_space=pltpu.SMEM)


def partial_shapes(rows):
    return [jax.ShapeDtypeStruct((n, rows, 128), BF16) for n in (2, 6, 8)]


def recurrent(order, gain, taps, decay, shift, shards, firsts):
    rows, count = shards[0].shape[0], len(firsts)
    wide = firsts[0].shape[1]
    depth = 8 * shards[0].shape[1] // count
    return pl.pallas_call(
        functools.partial(recurrent_body, count),
        in_specs=[smem()] + [vmem()] * (4 + 8 + count),
        out_specs=[vmem()] * 4,
        out_shape=partial_shapes(rows) + [jax.ShapeDtypeStruct((16, wide), F32)],
        scratch_shapes=[
            pltpu.VMEM((count, STEP, 128), BF16),
            pltpu.VMEM((depth * count, wide), BF16),
            pltpu.VMEM((16 * count, wide), BF16),
            pltpu.VMEM((16 * count, 128 * count), BF16),
            pltpu.VMEM((16, rows, 128), BF16),
        ],
        compiler_params=pltpu.CompilerParams(vmem_limit_bytes=20 << 20),
        cost_estimate=pl.CostEstimate(flops=3_500_000_000, bytes_accessed=12_000_000, transcendentals=2_000_000),
    )(order, gain, taps, decay, shift, *shards, *firsts)


def mixer(order, gain, scales, shards, pieces, swapped, batches):
    rows, count = shards[0].shape[0], len(pieces)
    half, wide = pieces[0].shape[0] // 2, pieces[0].shape[1]
    return pl.pallas_call(
        functools.partial(mixer_body, count, batches),
        in_specs=[smem()] + [vmem()] * (2 + 8 + count + len(swapped)),
        out_specs=[vmem()] * 3,
        out_shape=partial_shapes(rows),
        scratch_shapes=[
            pltpu.VMEM((count, STEP, 128), BF16),
            pltpu.VMEM((2 * half * count, wide), BF16),
            pltpu.VMEM((half * (wide // 128 + 1), 128 * count), BF16),
            pltpu.VMEM((16, rows, 128), BF16),
        ],
        compiler_params=pltpu.CompilerParams(vmem_limit_bytes=28 << 20),
        cost_estimate=pl.CostEstimate(flops=7_000_000_000, bytes_accessed=20_000_000, transcendentals=1_000_000),
    )(order, gain, scales, *shards, *pieces, *swapped)


def second_body(order, gate, up, down, scale, out):
    half = out.shape[0] // 2
    main = (out.shape[1] - 128) // 2
    rows = pl.ds(pl.multiple_of(order[56], half), half)
    out[:half, :main] = gate[rows, :main].astype(BF16)
    out[:half, main : 2 * main] = up[rows, :main].astype(BF16)
    tail = jnp.concatenate([gate[rows, main:], up[rows, main:]], axis=1)
    out[:half, 2 * main :] = tail.astype(BF16)
    for q in range(out.shape[1] // 128):
        block = down[half * q : half * (q + 1), :] * scale[...]
        out[half:, 128 * q : 128 * q + 128] = block.astype(BF16)


def second_shard(order, gate, up, down, scale):
    depth, wide = gate.shape
    return pl.pallas_call(
        second_body,
        in_specs=[smem()] + [vmem()] * 4,
        out_specs=vmem(),
        out_shape=jax.ShapeDtypeStruct((depth, 2 * wide), BF16),
        compiler_params=pltpu.CompilerParams(vmem_limit_bytes=8 << 20),
        cost_estimate=pl.CostEstimate(flops=200_000_000, bytes_accessed=1_500_000, transcendentals=0),
    )(order, gate, up, down, scale)


def first_body(gate, up, recur, inject, out, scale, scales, first):
    depth = gate.shape[0]
    fourth = out.shape[0] // 4
    first[:depth, :256] = gate[...].astype(BF16)
    first[:depth, 256:] = up[...].astype(BF16)
    first[depth : depth + 16, :256] = recur[...].astype(BF16)
    first[depth : depth + 16, 256:] = inject[...].astype(BF16)
    first[depth + 16 : depth + 32, :] = scales[...]
    for q in range(4):
        block = out[fourth * q : fourth * (q + 1), :] * scale[...]
        first[depth + 32 :, 128 * q : 128 * q + 128] = block.astype(BF16)


def first_shard(gate, up, recur, inject, out, scale, scales):
    height = gate.shape[0] + 32 + out.shape[0] // 4
    return pl.pallas_call(
        first_body,
        in_specs=[vmem()] * 7,
        out_specs=vmem(),
        out_shape=jax.ShapeDtypeStruct((height, 512), BF16),
        compiler_params=pltpu.CompilerParams(vmem_limit_bytes=8 << 20),
        cost_estimate=pl.CostEstimate(flops=200_000_000, bytes_accessed=900_000, transcendentals=0),
    )(gate, up, recur, inject, out, scale, scales)


def spread(scale, here, count):
    return jnp.where(here, scale[None, :], 0.0).reshape(count * scale.shape[0])


def on_device(
    groups,
    fs,
    tp,
    tokens,
    recurrent_norm_gain,
    channel_norm_gain,
    gate_projection_weight,
    gate_column_scale,
    input_projection_weight,
    input_column_scale,
    convolution_kernel,
    recurrence_gate_weight,
    recurrence_column_scale,
    input_gate_weight,
    input_gate_column_scale,
    channel_decay_param,
    position_decay_shift,
    output_projection_weight,
    output_column_scale,
    mixer_gate_weight,
    mixer_gate_column_scale,
    up_projection_weight,
    up_column_scale,
    down_projection_weight,
    down_column_scale,
):
    g, z, t = lax.axis_index("grp"), lax.axis_index("fs"), lax.axis_index("tp")
    table = jnp.asarray(tables(groups, fs, tp).reshape(groups * fs * tp, -1))
    table = lax.dynamic_index_in_dim(table, (g * fs + z) * tp + t, 0, keepdims=False)
    here = lax.broadcasted_iota(jnp.int32, (fs, 1), 0) == z
    main = mixer_gate_weight.shape[1] // 128 * 128

    small = [gate_column_scale, input_column_scale, recurrence_column_scale[0], input_gate_column_scale[0]]
    small = jnp.concatenate([spread(s, here, fs) for s in small]).reshape(2, 512)
    a, b = spread(mixer_gate_column_scale, here, fs), spread(up_column_scale, here, fs)
    large = jnp.concatenate([a[:main], b[:main], a[main:], b[main:], jnp.zeros((128,), F32)]).reshape(3, 512)
    small_high, large_high = small.astype(BF16), large.astype(BF16)
    small_low = (small - small_high.astype(F32)).astype(BF16)
    large_low = (large - large_high.astype(F32)).astype(BF16)
    scales = [small_high[0:1], small_low[0:1], small_high[1:2], small_low[1:2], large_high, large_low]
    scales = jnp.concatenate(scales + [jnp.zeros((6, 512), BF16)], axis=0)
    decay = -8.0 * jax.nn.softplus(-channel_decay_param)[None, :]
    shift = position_decay_shift[:, None]

    first = first_shard(
        gate_projection_weight,
        input_projection_weight,
        recurrence_gate_weight[0],
        input_gate_weight[0],
        output_projection_weight,
        output_column_scale[None, :],
        scales,
    )
    second = second_shard(
        table, mixer_gate_weight, up_projection_weight, down_projection_weight, down_column_scale[None, :]
    )
    half = second.shape[0] // 2
    swap, lane = tp_perms(tp)
    pair = [(i, i ^ 1) for i in range(groups)]
    firsts, seconds = [first] + [None] * (fs - 1), [second] + [None] * (fs - 1)
    swapped, batches, waiting, events = [], [], [0], {}

    def hop(pieces, step, *event):
        up, down = pieces[step - 1], pieces[1 - step]
        up, down, *_ = lax.optimization_barrier((up, down, *event))
        up, down = ring_step(up, down, step, fs)
        pieces[step] = up
        if down is not None:
            pieces[fs - step] = down

    def across(*steps):
        group = [j for step in steps for j in sorted({step, (fs - step) % fs})]
        batches.append(tuple(group))
        block = jnp.concatenate([seconds[j][:half] for j in group], axis=0)
        swapped.append(lax.ppermute(block, "grp", pair))

    def forward(step, *event):
        hop(firsts, step, *event)

    def side(step, *event):
        hop(seconds, step, *event)

    near = lax.ppermute(tokens, "tp", lane)
    partner = lax.ppermute(tokens, "tp", swap)
    forward(1)
    side(1, firsts[0])
    forward(2)
    forward(3, near, partner)
    near_other = lax.ppermute(after(partner, firsts[2]), "tp", lane)
    far = lax.ppermute(near, "tp", lane)
    side(2, firsts[2])
    forward(4, seconds[1])
    across(0, 1)
    side(3, firsts[3])
    forward(5, seconds[2], near_other, far)
    crossed = [lax.ppermute(v, "tp", swap) for v in (near, near_other, far)]
    side(4, firsts[5])
    forward(6, seconds[3], swapped[0])
    across(2, 3)
    forward(7, *crossed)
    side(5, firsts[6])
    forward(8, seconds[4])
    side(6, firsts[8], firsts[fs - 7])
    shards = [tokens, partner, near, near_other, far] + crossed
    shards[0] = after(tokens, seconds[5], swapped[1])
    *partial, passed = recurrent(
        table,
        recurrent_norm_gain.reshape(tp, 1, -1),
        convolution_kernel,
        decay,
        shift,
        shards,
        firsts,
    )
    across(4, 5)
    terms = tp_scatter(partial, tp, events)
    side(7, events["swapped"])
    side(8, events["far"])
    across(6, 7, 8)
    hidden = add_terms(after(tokens, seconds[7], swapped[2]), terms)
    shards = tp_gather(hidden, tp)
    partial = mixer(table, channel_norm_gain.reshape(tp, 1, -1), passed, shards, seconds, swapped, batches)
    return add_terms(hidden, tp_scatter(partial, tp, events))


def solution(mesh):
    placed = (
        P(("grp", "fs"), "tp"),
        P(),
        P(),
        P("fs", "tp"),
        P(("tp", "fs")),
        P("fs", "tp"),
        P(("tp", "fs")),
        P(None, "tp"),
        P("tp", "fs", None),
        P("tp", "fs"),
        P("tp", "fs", None),
        P("tp", "fs"),
        P("tp"),
        P(("grp", "fs")),
        P("tp", "fs"),
        P("fs"),
        P("fs", "tp"),
        P(("tp", "fs")),
        P("fs", "tp"),
        P(("tp", "fs")),
        P("tp", "fs"),
        P("fs"),
    )
    body = functools.partial(on_device, mesh.shape["grp"], mesh.shape["fs"], mesh.shape["tp"])
    return jax.shard_map(
        body, mesh=mesh, in_specs=placed, out_specs=P(("grp", "fs"), "tp"), check_vma=False
    )
```

```python
import functools

import jax
import jax.numpy as jnp
import numpy as np
from jax import lax
from jax.experimental import pallas as pl
from jax.experimental.pallas import tpu as pltpu
from jax.sharding import PartitionSpec as P


SEQ_LEN = 128
EPS = 1e-06
F32 = jnp.float32
BF16 = jnp.bfloat16


def fs_ring(size):
    forward = [(i, (i + 1) % size) for i in range(size)]
    backward = [(i, (i - 1) % size) for i in range(size)]
    return forward, backward


def ring_step(up, down, step, size):
    forward, backward = fs_ring(size)
    up = lax.ppermute(up, "fs", forward)
    return up, (lax.ppermute(down, "fs", backward) if step < size - step else None)


def after(value, *events):
    return lax.optimization_barrier((value, *events))[0]


def tp_perms(size):
    chips = size // 2
    swap = [(i, i ^ 1) for i in range(size)]
    lane = [(i, ((i // 2 + (1 if i % 2 == 0 else -1)) % chips) * 2 + i % 2) for i in range(size)]
    return swap, lane


def tp_gather(own, size, *events):
    swap, lane = tp_perms(size)
    near = lax.ppermute(own, "tp", lane)
    partner = lax.ppermute(own, "tp", swap)
    near_other = lax.ppermute(partner, "tp", lane)
    far = lax.ppermute(near, "tp", lane)
    return [
        own,
        partner,
        near,
        near_other,
        far,
        lax.ppermute(near, "tp", swap),
        lax.ppermute(near_other, "tp", swap),
        lax.ppermute(after(far, *events), "tp", swap),
    ]


def gather_order(index, size):
    chips = size // 2
    chip, core = index // 2, index % 2
    sign = 1 - 2 * core
    behind, ahead = (chip - sign) % chips, (chip + sign) % chips
    across = (chip + 2) % chips
    return [
        2 * chip + core,
        2 * chip + 1 - core,
        2 * behind + core,
        2 * behind + 1 - core,
        2 * across + core,
        2 * ahead + 1 - core,
        2 * ahead + core,
        2 * across + 1 - core,
    ]


def scatter_order(index, size):
    chips = size // 2
    chip, core = index // 2, index % 2
    sign = 1 - 2 * core
    ahead, behind = (chip + sign) % chips, (chip - sign) % chips
    across = (chip + 2) % chips
    return [
        2 * across + 1 - core,
        2 * behind + 1 - core,
        2 * behind + core,
        2 * chip + 1 - core,
        2 * across + core,
        2 * ahead + core,
        2 * ahead + 1 - core,
        2 * chip + core,
    ]


def tables(groups, fs, tp):
    rows = []
    for g in range(groups):
        for z in range(fs):
            for t in range(tp):
                order = gather_order(t, tp)
                blocks = [(z - (2 * p + h)) % fs for p in order for h in range(2)]
                where = np.argsort(scatter_order(t, tp))
                absolute = [(z - j) % fs for j in range(fs)]
                laid = [2 * int(where[a // 2]) + a % 2 for a in absolute]
                rows.append(order + blocks + laid + [16 * a for a in absolute] + [64 * (g % 2), z])
    return np.asarray(rows, np.int32).reshape(groups, fs, tp, -1)


def tp_scatter(partial, size, first=(), last=()):
    swap, lane = tp_perms(size)
    given_far, given_rest, kept = partial
    taken_far = lax.ppermute(given_far, "tp", swap)
    taken = lax.ppermute(given_rest, "tp", swap)
    taken_far = after(taken_far, *first)
    passed_on = (kept[0:2].astype(F32) + taken_far.astype(F32)).astype(BF16)
    far = lax.ppermute(passed_on, "tp", lane)
    taken = after(taken, passed_on)
    sent = (kept[4:6].astype(F32) + taken[2:4].astype(F32)).astype(BF16)
    other = lax.ppermute(sent, "tp", lane)
    near = kept[2:4].astype(F32) + taken[0:2].astype(F32)
    far = after(far, sent, *last)
    mine = lax.ppermute((near + far.astype(F32)).astype(BF16), "tp", lane)
    other = lax.ppermute(other, "tp", swap)
    return kept, taken, mine, other


def add_body(base, kept, taken, mine, other, out):
    for half in range(2):
        lanes = slice(128 * half, 128 * half + 128)
        total = kept[half].astype(F32) + taken[half].astype(F32)
        total = total + mine[half].astype(F32) + other[half].astype(F32)
        out[:, lanes] = (base[:, lanes].astype(F32) + total).astype(BF16)


def add_terms(base, terms):
    rows = base.shape[0]
    step = rows // 2

    def pair(k):
        return pl.BlockSpec((2, step, 128), lambda i: (k, i, 0))

    flat = pl.BlockSpec((step, 256), lambda i: (i, 0))
    return pl.pallas_call(
        add_body,
        grid=(rows // step,),
        in_specs=[flat, pair(3), pair(2), pair(0), pair(0)],
        out_specs=flat,
        out_shape=jax.ShapeDtypeStruct(base.shape, BF16),
        compiler_params=pltpu.CompilerParams(vmem_limit_bytes=8 << 20),
        cost_estimate=pl.CostEstimate(flops=rows * 256 * 2000, bytes_accessed=rows * 256 * 12, transcendentals=0),
    )(base, *terms)


def norm_into(order, gain, shards, xs, rows):
    width = shards[0].shape[1] * len(shards)
    square = None
    for shard in shards:
        v = shard[rows, :].astype(F32)
        s = v * v
        s = s[:, :128] + s[:, 128:]
        square = s if square is None else square + s
    inverse = lax.rsqrt(jnp.sum(square, axis=1, keepdims=True) * (1.0 / width) + EPS)
    for n, shard in enumerate(shards):
        v = shard[rows, :].astype(F32) * inverse * gain[order[n]]
        v = v.astype(BF16)
        for half in range(2):
            xs[order[8 + 2 * n + half]] = v[:, 128 * half : 128 * half + 128]


def lay_down(order, laid, rows, left, right, count):
    for j in range(0, count, 2):
        columns = slice(128 * j, 128 * j + 256)
        result = jnp.dot(left, right[:, columns], preferred_element_type=F32).astype(BF16)
        laid[order[24 + j], rows, :] = result[:, :128]
        laid[order[24 + j + 1], rows, :] = result[:, 128:]


STEP = 3 * SEQ_LEN


def recurrent_body(count, order, gain, taps, decay, shift, *refs):
    shards, refs = refs[:8], refs[8:]
    firsts, refs = refs[:count], refs[count:]
    given_far, given, kept, passed, xs, weight, gates, out, laid = refs
    total = laid.shape[1]
    depth = weight.shape[0] // count
    fourth = gates.shape[0] // 4
    scales = None
    for j, first in enumerate(firsts):
        weight[depth * j : depth * (j + 1), :] = first[:depth, :]
        at = pl.multiple_of(order[40 + j], 16)
        gates[pl.ds(at, 16), :] = first[depth : depth + 16, :]
        part = first[depth + 16 : depth + 32, :].astype(F32)
        scales = part if scales is None else scales + part
        for q in range(4):
            block = first[depth + 32 : depth + 32 + fourth, 128 * q : 128 * q + 128]
            out[fourth * q : fourth * (q + 1), 128 * j : 128 * j + 128] = block
    passed[...] = scales
    branch_scale = scales[0:1] + scales[1:2]
    gate_scale = scales[2:3] + scales[3:4]

    def chunk(r, carry):
        rows = pl.ds(pl.multiple_of(r * STEP, STEP), STEP)
        norm_into(order, gain, shards, xs, rows)
        left = jnp.concatenate([xs[j] for j in range(count)], axis=1)
        sums = jnp.dot(left, weight[...], preferred_element_type=F32) * branch_scale
        gate_branch = sums[:, :256].astype(BF16).astype(F32)
        branch = sums[:, 256:].astype(BF16).astype(F32)
        place = lax.broadcasted_iota(jnp.int32, (STEP, 256), 0) % SEQ_LEN
        conv = branch * taps[0:1, :]
        for k in range(1, 4):
            moved = jnp.where(place >= k, pltpu.roll(branch, k, 0), 0.0)
            conv = conv + moved * taps[k : k + 1, :]
        conv16 = conv.astype(BF16)
        conv = conv16.astype(F32)
        both = jnp.dot(conv16, gates[...], preferred_element_type=F32) * gate_scale
        both = 1.0 / (1.0 + jnp.exp(-both))
        log_keep = both[:, :256] * decay[...] + shift[rows, :]
        twice = 2.0 * log_keep
        series = 1.0 + twice * (1.0 / 7)
        for d in (6, 5, 4, 3, 2):
            series = 1.0 + twice * (1.0 / d) * series
        lost = jnp.where(twice > -0.35, -twice * series, 1.0 - jnp.exp(twice))
        first = place == 0
        state = conv * both[:, 256:] * jnp.where(first, 1.0, jnp.sqrt(lost))
        keep = jnp.where(first, 0.0, jnp.exp(log_keep))
        d = 1
        while d < SEQ_LEN:
            state = state + keep * pltpu.roll(state, d, 0)
            if 2 * d < SEQ_LEN:
                keep = keep * pltpu.roll(keep, d, 0)
            d *= 2
        mixed = (jax.nn.gelu(gate_branch) * state).astype(BF16)
        lay_down(order, laid, rows, mixed, out, count)
        return carry

    lax.fori_loop(0, total // STEP, chunk, 0)
    given_far[...] = laid[:2]
    given[...] = laid[2:8]
    kept[...] = laid[8:]


def mixer_body(count, batches, order, gain, scales, *refs):
    shards, refs = refs[:8], refs[8:]
    pieces, refs = refs[:count], refs[count:]
    swapped, refs = refs[: len(batches)], refs[len(batches) :]
    given_far, given, kept, xs, weight, down, laid = refs
    total = laid.shape[1]
    half = weight.shape[0] // count // 2
    wide = weight.shape[1]
    main = (wide - 128) // 2
    own = pl.multiple_of(order[56], half)
    lanes = wide // 128
    for j, piece in enumerate(pieces):
        weight[pl.ds(2 * half * j + own, half), :] = piece[:half, :]
        columns = slice(128 * j, 128 * j + 128)
        for q in range(lanes):
            at = half * (q if q < lanes - 1 else q + 1)
            down[at : at + half, columns] = piece[half:, 128 * q : 128 * q + 128]
        down[main : main + half, columns] = jnp.zeros((half, 128), BF16)
    for batch, group in zip(swapped, batches):
        for i, j in enumerate(group):
            weight[pl.ds(2 * half * j + half - own, half), :] = batch[half * i : half * (i + 1), :]
    at = [scales[4 + k : 5 + k, :] + scales[7 + k : 8 + k, :] for k in range(3)]
    scale = jnp.concatenate(at, axis=1)[:, :wide]

    def chunk(r, carry):
        rows = pl.ds(pl.multiple_of(r * STEP, STEP), STEP)
        norm_into(order, gain, shards, xs, rows)
        left = jnp.concatenate([xs[j] for j in range(count)], axis=1)
        sums = jnp.dot(left, weight[...], preferred_element_type=F32) * scale
        swish, upward, tail = sums[:, :main], sums[:, main : 2 * main], sums[:, 2 * main :]
        active = (swish / (1.0 + jnp.exp(-swish)) * upward).astype(BF16)
        turned = pltpu.roll(tail, 64, 1)
        lane = lax.broadcasted_iota(jnp.int32, tail.shape, 1)
        last = jnp.where(lane >= 64, turned / (1.0 + jnp.exp(-turned)) * tail, 0.0).astype(BF16)
        active = jnp.concatenate([active, last], axis=1)
        lay_down(order, laid, rows, active, down, count)
        return carry

    lax.fori_loop(0, total // STEP, chunk, 0)
    given_far[...] = laid[:2]
    given[...] = laid[2:8]
    kept[...] = laid[8:]


def vmem():
    return pl.BlockSpec(memory_space=pltpu.VMEM)


def smem():
    return pl.BlockSpec(memory_space=pltpu.SMEM)


def partial_shapes(rows):
    return [jax.ShapeDtypeStruct((n, rows, 128), BF16) for n in (2, 6, 8)]


def recurrent(order, gain, taps, decay, shift, shards, firsts):
    rows, count = shards[0].shape[0], len(firsts)
    wide = firsts[0].shape[1]
    depth = 8 * shards[0].shape[1] // count
    return pl.pallas_call(
        functools.partial(recurrent_body, count),
        in_specs=[smem()] + [vmem()] * (4 + 8 + count),
        out_specs=[vmem()] * 4,
        out_shape=partial_shapes(rows) + [jax.ShapeDtypeStruct((16, wide), F32)],
        scratch_shapes=[
            pltpu.VMEM((count, STEP, 128), BF16),
            pltpu.VMEM((depth * count, wide), BF16),
            pltpu.VMEM((16 * count, wide), BF16),
            pltpu.VMEM((16 * count, 128 * count), BF16),
            pltpu.VMEM((16, rows, 128), BF16),
        ],
        compiler_params=pltpu.CompilerParams(vmem_limit_bytes=20 << 20),
        cost_estimate=pl.CostEstimate(flops=3_500_000_000, bytes_accessed=12_000_000, transcendentals=2_000_000),
    )(order, gain, taps, decay, shift, *shards, *firsts)


def mixer(order, gain, scales, shards, pieces, swapped, batches):
    rows, count = shards[0].shape[0], len(pieces)
    half, wide = pieces[0].shape[0] // 2, pieces[0].shape[1]
    return pl.pallas_call(
        functools.partial(mixer_body, count, batches),
        in_specs=[smem()] + [vmem()] * (2 + 8 + count + len(swapped)),
        out_specs=[vmem()] * 3,
        out_shape=partial_shapes(rows),
        scratch_shapes=[
            pltpu.VMEM((count, STEP, 128), BF16),
            pltpu.VMEM((2 * half * count, wide), BF16),
            pltpu.VMEM((half * (wide // 128 + 1), 128 * count), BF16),
            pltpu.VMEM((16, rows, 128), BF16),
        ],
        compiler_params=pltpu.CompilerParams(vmem_limit_bytes=28 << 20),
        cost_estimate=pl.CostEstimate(flops=7_000_000_000, bytes_accessed=20_000_000, transcendentals=1_000_000),
    )(order, gain, scales, *shards, *pieces, *swapped)


def second_body(order, gate, up, down, scale, out):
    half = out.shape[0] // 2
    main = (out.shape[1] - 128) // 2
    rows = pl.ds(pl.multiple_of(order[56], half), half)
    out[:half, :main] = gate[rows, :main].astype(BF16)
    out[:half, main : 2 * main] = up[rows, :main].astype(BF16)
    tail = jnp.concatenate([gate[rows, main:], up[rows, main:]], axis=1)
    out[:half, 2 * main :] = tail.astype(BF16)
    for q in range(out.shape[1] // 128):
        block = down[half * q : half * (q + 1), :] * scale[...]
        out[half:, 128 * q : 128 * q + 128] = block.astype(BF16)


def second_shard(order, gate, up, down, scale):
    depth, wide = gate.shape
    return pl.pallas_call(
        second_body,
        in_specs=[smem()] + [vmem()] * 4,
        out_specs=vmem(),
        out_shape=jax.ShapeDtypeStruct((depth, 2 * wide), BF16),
        compiler_params=pltpu.CompilerParams(vmem_limit_bytes=8 << 20),
        cost_estimate=pl.CostEstimate(flops=200_000_000, bytes_accessed=1_500_000, transcendentals=0),
    )(order, gate, up, down, scale)


def split(row):
    high = row.astype(BF16)
    return high, (row - high.astype(F32)).astype(BF16)


def first_body(z, *refs):
    count = len(refs) // 2 - 1
    sources, first, held, sems = refs[:count], refs[count], refs[count + 1 : -1], refs[-1]
    copies = [pltpu.make_async_copy(a, b, sems.at[n]) for n, (a, b) in enumerate(zip(sources, held))]
    for copy in copies:
        copy.start()
    for copy in copies:
        copy.wait()
    gate, up, recur, inject, out, scale, *columns = held
    depth = gate.shape[0]
    fourth = out.shape[0] // 4

    def placed(column, width):
        own = column.shape[1]
        row = jnp.concatenate([column[...], jnp.zeros((1, width - own), F32)], axis=1)
        return pltpu.roll(jnp.broadcast_to(row, (8, width)), z[0] * own, 1)[0:1]

    small = [placed(c, 256) for c in columns[:4]]
    large = [placed(c, 768) for c in columns[4:]]
    rows = []
    for pair in (small[:2], small[2:]):
        rows += split(jnp.concatenate(pair, axis=1))
    tail = jnp.concatenate([large[0][:, 640:704], large[1][:, 640:704]], axis=1)
    wide = jnp.concatenate([large[0][:, :640], large[1][:, :640], tail, jnp.zeros((1, 128), F32)], axis=1)
    high, low = split(wide)
    for part in (high, low):
        rows += [part[:, 512 * k : 512 * (k + 1)] for k in range(3)]
    rows.append(jnp.zeros((6, 512), BF16))
    first[:depth, :256] = gate[...].astype(BF16)
    first[:depth, 256:] = up[...].astype(BF16)
    first[depth : depth + 16, :256] = recur[...].astype(BF16)
    first[depth : depth + 16, 256:] = inject[...].astype(BF16)
    at = depth + 16
    for row in rows:
        first[at : at + row.shape[0], :] = row
        at += row.shape[0]
    for q in range(4):
        block = out[fourth * q : fourth * (q + 1), :] * scale[...]
        first[depth + 32 :, 128 * q : 128 * q + 128] = block.astype(BF16)


def first_shard(z, *sources):
    height = sources[0].shape[0] + 32 + sources[4].shape[0] // 4
    sources = [pltpu.with_memory_space_constraint(v, pltpu.HBM) for v in sources]
    return pl.pallas_call(
        first_body,
        in_specs=[smem()] + [pl.BlockSpec(memory_space=pltpu.HBM)] * len(sources),
        out_specs=vmem(),
        out_shape=jax.ShapeDtypeStruct((height, 512), BF16),
        scratch_shapes=[pltpu.VMEM(v.shape, v.dtype) for v in sources]
        + [pltpu.SemaphoreType.DMA((len(sources),))],
        compiler_params=pltpu.CompilerParams(vmem_limit_bytes=8 << 20),
        cost_estimate=pl.CostEstimate(flops=200_000_000, bytes_accessed=0, transcendentals=0),
    )(z, *sources)


def on_device(
    groups,
    fs,
    tp,
    tokens,
    recurrent_norm_gain,
    channel_norm_gain,
    gate_projection_weight,
    gate_column_scale,
    input_projection_weight,
    input_column_scale,
    convolution_kernel,
    recurrence_gate_weight,
    recurrence_column_scale,
    input_gate_weight,
    input_gate_column_scale,
    channel_decay_param,
    position_decay_shift,
    output_projection_weight,
    output_column_scale,
    mixer_gate_weight,
    mixer_gate_column_scale,
    up_projection_weight,
    up_column_scale,
    down_projection_weight,
    down_column_scale,
):
    g, z, t = lax.axis_index("grp"), lax.axis_index("fs"), lax.axis_index("tp")
    table = jnp.asarray(tables(groups, fs, tp).reshape(groups * fs * tp, -1))
    table = lax.dynamic_index_in_dim(table, (g * fs + z) * tp + t, 0, keepdims=False)
    decay = -8.0 * jax.nn.softplus(-channel_decay_param)[None, :]
    shift = position_decay_shift[:, None]

    columns = [
        output_column_scale,
        gate_column_scale,
        input_column_scale,
        recurrence_column_scale[0],
        input_gate_column_scale[0],
        mixer_gate_column_scale,
        up_column_scale,
    ]
    first = first_shard(
        z.astype(jnp.int32).reshape(1),
        gate_projection_weight,
        input_projection_weight,
        recurrence_gate_weight[0],
        input_gate_weight[0],
        output_projection_weight,
        *[v[None, :] for v in columns],
    )
    second = second_shard(
        table, mixer_gate_weight, up_projection_weight, down_projection_weight, down_column_scale[None, :]
    )
    half = second.shape[0] // 2
    swap, lane = tp_perms(tp)
    pair = [(i, i ^ 1) for i in range(groups)]
    firsts, seconds = [first] + [None] * (fs - 1), [second] + [None] * (fs - 1)
    swapped, batches = [], []

    def hop(pieces, step, *event):
        up, down = pieces[step - 1], pieces[1 - step]
        up, down, *_ = lax.optimization_barrier((up, down, *event))
        up, down = ring_step(up, down, step, fs)
        pieces[step] = up
        if down is not None:
            pieces[fs - step] = down

    def across(*steps):
        group = [j for step in steps for j in sorted({step, (fs - step) % fs})]
        batches.append(tuple(group))
        block = jnp.concatenate([seconds[j][:half] for j in group], axis=0)
        swapped.append(lax.ppermute(block, "grp", pair))

    def forward(step, *event):
        hop(firsts, step, *event)

    def side(step, *event):
        hop(seconds, step, *event)

    near = lax.ppermute(tokens, "tp", lane)
    partner = lax.ppermute(tokens, "tp", swap)
    forward(1)
    side(1, firsts[0])
    forward(2)
    forward(3, near, partner)
    near_other = lax.ppermute(after(partner, firsts[2]), "tp", lane)
    far = lax.ppermute(near, "tp", lane)
    side(2, firsts[2])
    forward(4, seconds[1])
    across(0, 1)
    side(3, firsts[3])
    forward(5, seconds[2], near_other, far)
    crossed = [lax.ppermute(v, "tp", swap) for v in (near, near_other, far)]
    side(4, firsts[5])
    forward(6, seconds[3], swapped[0])
    across(2, 3)
    forward(7, *crossed)
    side(5, firsts[6])
    forward(8, seconds[4])
    across(4)
    side(6, firsts[8], firsts[fs - 7])
    shards = [tokens, partner, near, near_other, far] + crossed
    shards[0] = after(tokens, seconds[5], swapped[1])
    *partial, passed = recurrent(
        table,
        recurrent_norm_gain.reshape(tp, 1, -1),
        convolution_kernel,
        decay,
        shift,
        shards,
        firsts,
    )
    across(5, 6)
    side(7)
    side(8)
    across(7, 8)
    terms = tp_scatter(partial, tp, (seconds[6], seconds[fs - 6]))
    hidden = add_terms(tokens, terms)
    shards = tp_gather(hidden, tp, seconds[8], swapped[3])
    partial = mixer(table, channel_norm_gain.reshape(tp, 1, -1), passed, shards, seconds, swapped, batches)
    return add_terms(hidden, tp_scatter(partial, tp))


def solution(mesh):
    placed = (
        P(("grp", "fs"), "tp"),
        P(),
        P(),
        P("fs", "tp"),
        P(("tp", "fs")),
        P("fs", "tp"),
        P(("tp", "fs")),
        P(None, "tp"),
        P("tp", "fs", None),
        P("tp", "fs"),
        P("tp", "fs", None),
        P("tp", "fs"),
        P("tp"),
        P(("grp", "fs")),
        P("tp", "fs"),
        P("fs"),
        P("fs", "tp"),
        P(("tp", "fs")),
        P("fs", "tp"),
        P(("tp", "fs")),
        P("tp", "fs"),
        P("fs"),
    )

    def body(*args):
        return on_device(mesh.shape["grp"], mesh.shape["fs"], mesh.shape["tp"], *args)

    return jax.shard_map(
        body, mesh=mesh, in_specs=placed, out_specs=P(("grp", "fs"), "tp"), check_vma=False
    )
```
